32 devices in a mesh: dp: 4 (over y, x), kv: 4 (over z), tp: 2 (over core).
Axes of the slice: x: 2, y: 2, z: 4, core: 2. Of those that a mesh axis runs over, the one named last changes fastest.
Arguments:
- piece_tokens: bfloat16 [2048, 2048], P(('dp', 'kv')), parts along dimension 0, may hold values from -6 to 6
- step_tokens: bfloat16 [16, 2048], P(('dp', 'kv')), parts along dimension 0, may hold values from -6 to 6
- norm_gain: float32 [2048], replicated, may hold values from 0.1 to 1.9
- query_weight: bfloat16 [2048, 1024], P(None, 'tp'), may hold values from -0.125 to 0.125
- key_weight: bfloat16 [2048, 1024], P(None, 'tp'), may hold values from -0.125 to 0.125
- value_weight: bfloat16 [2048, 1024], P(None, 'tp'), may hold values from -0.125 to 0.125
- gate_weight: bfloat16 [2048, 16], replicated, may hold values from -0.125 to 0.125
- gate_bias: float32 [16], replicated, may hold values from 3 to 10.5
- out_weight: bfloat16 [1024, 2048], P(None, 'tp'), may hold values from -0.1875 to 0.1875
- cache_keys: bfloat16 [8192, 1024], P(('dp', 'kv'), 'tp'), parts along dimension 0, may hold values from -320 to 320
- cache_values: bfloat16 [8192, 1024], P(('dp', 'kv'), 'tp'), parts along dimension 0, may hold values from -10 to 10
- cache_decay: float32 [16, 8192], P('tp', ('dp', 'kv')), parts along dimension 1, may hold values from -696.32 to 0, as said below
- decay_total: float32 [64], P('dp'), parts along dimension 0, may hold values from -696.32 to 0, as said below
- step_keys: bfloat16 [16, 1024, 1024], P(('dp', 'kv'), None, 'tp'), parts along dimension 0, may hold values from -6 to 6
- step_values: bfloat16 [16, 1024, 1024], P(('dp', 'kv'), None, 'tp'), parts along dimension 0, may hold values from -6 to 6
- step_gates: float32 [16, 16, 1024], P(('dp', 'kv'), 'tp'), parts along dimension 0, may hold values from -0.34 to 0
- step_lengths: int32 [16], P(('dp', 'kv')), parts along dimension 0, may hold values from 1 to 1024, 2048 in all
Outputs:
- piece_out: bfloat16 [2048, 2048], P(('dp', 'kv'), 'tp'), parts along dimension 0
- step_out: bfloat16 [16, 2048], P(('dp', 'kv'), 'tp'), parts along dimension 0
The draws below stay inside these ranges and needn't reach their ends.
There are 4 independent parts, one for each index of `dp`. The reference program is written for one: setup_inputs(seed, part) draws one part's arguments, and reference() takes and returns one part's arrays. A program takes and returns all parts, laid end to end along the dimension named above; an argument that names none is the same for every part. Nothing has to cross between parts.
Inputs may be any that keep to these rules, and one draw needn't show every extreme that they name: `cache_decay`: cumulative values never rise along the positions and start at one gate below zero. `decay_total`: equal to the cumulative value of the last cached position. `step_lengths`: each length is 1 to 1024; the largest is exactly 1024; positions at or past a length are unused.
All inputs are finite; a program needn't handle non-finite values.
Results may differ from the reference program's by a relative error of at most 0.0095.
The reference program's roundings to bfloat16 on the way count: a program that leaves them out, or rounds other values in their place, can miss the bound.
Values may be sent and summed in bfloat16 or wider, within the bound.
A program may use at most 128 MiB of HBM per device.

```python
import math
import jax
import jax.numpy as jnp
import numpy as np
from jax import lax

D = 2048
HEADS = 16
HEAD = 64
PIECE_DEV = 128
DEC_LEN = 1024
CACHE_DEV = 512
PIECE = 512
CACHE = 2048
DEC = 4
N_KV = 4


def fast_heads(key):
    ranking = jax.random.permutation(jax.random.fold_in(key, 13), HEADS)
    fast_count = HEADS // 2
    return ranking < fast_count


def gate_values(key, leading, span, block):
    fast_mask = fast_heads(key)
    base_rate = jnp.where(fast_mask, 0.03, 5e-05).astype(jnp.float32)
    factor = 0.5 + jax.random.uniform(jax.random.fold_in(key, 12), (leading, 1, span // block), jnp.float32)
    factor = jnp.repeat(factor, block, axis=2)
    noise_key = jax.random.fold_in(key, 11)
    spread = jnp.clip(jax.random.normal(noise_key, (leading, HEADS, span), jnp.float32), -4.0, 4.0) * 0.5
    return -base_rate[None, :, None] * factor * jnp.exp(spread)


def prompt_decay(key):
    gates_drawn = gate_values(jax.random.fold_in(key, 5), 1, CACHE, CACHE_DEV)[0]
    return jnp.cumsum(gates_drawn, axis=1)


def draw_gate_bias(key, part):
    offsets = jax.random.uniform(jax.random.fold_in(key, 3), (HEADS,), jnp.float32)
    fast_mask = fast_heads(jax.random.fold_in(key, 4))
    return jnp.where(fast_mask, 3.0 + offsets, 9.5 + offsets)


def draw_cache_keys(key, part):
    base_keys = jnp.clip(jax.random.normal(jax.random.fold_in(key, 21), (CACHE, HEADS * HEAD), jnp.float32), -4.0, 4.0)
    return base_keys.astype(jnp.bfloat16)


def draw_cache_values(key, part):
    noise_key = jax.random.fold_in(key, 31)
    noise = jnp.clip(jax.random.normal(noise_key, (CACHE, HEADS * HEAD), jnp.float32), -4.0, 4.0)
    block_means = jnp.clip(jax.random.normal(jax.random.fold_in(key, 32), (CACHE // CACHE_DEV, HEADS * HEAD), jnp.float32), -4.0, 4.0) * 1.5
    return (noise + jnp.repeat(block_means, CACHE_DEV, axis=0)).astype(jnp.bfloat16)


def draw_cache_decay(key, part):
    return prompt_decay(key)


def draw_decay_total(key, part):
    return prompt_decay(key)[:, -1]


def draw_step_gates(key, part):
    return gate_values(jax.random.fold_in(key, 9), DEC, DEC_LEN, DEC_LEN)


def steps_of(rng, shape, pieces, smallest, high):
    level = 1.0
    for position, blocks in pieces:
        heights = jax.random.uniform(jax.random.fold_in(jax.random.fold_in(rng, 6), position), (blocks,), jnp.float32, smallest / len(pieces), high / len(pieces))
        level = level * jnp.repeat(jnp.exp(heights), shape[position] // blocks).reshape((-1,) + (1,) * (len(shape) - 1 - position))
    return level


def length_profile(count, total, limit, skew):
    portions = [(1 << 20) // math.isqrt(rank ** skew) + 1 for rank in range(2, count + 1)]
    spare, counts = total - limit - (count - 1), [1] * (count - 1)
    while spare > 0:
        free = [i for i in range(count - 1) if counts[i] < limit]
        pool, left = sum([portions[i] for i in free]), spare
        for i in free:
            addition = min(limit - counts[i], max(1, left * portions[i] // pool), spare)
            counts[i] = counts[i] + addition
            spare = spare - addition
    return np.array([limit] + counts)


def ragged(rng, amount, total, bound, lean):
    if amount == 2:
        one = jax.random.randint(rng, (), max(1, total - bound), min(bound, total - 1) + 1)
        return jnp.stack([one, total - one])
    sizes = jnp.asarray(length_profile(amount, total, bound, lean), jnp.int32)
    couples = (amount - 1) // 2
    donor, taker = sizes[1:1 + 2 * couples:2], sizes[2:2 + 2 * couples:2]
    room = jnp.minimum(donor - 1, bound - taker)
    shifted = jax.random.randint(jax.random.fold_in(rng, 1), (couples,), 0, 1 << 20) % (room + 1)
    sizes = sizes.at[1:1 + 2 * couples:2].set(donor - shifted).at[2:2 + 2 * couples:2].set(taker + shifted)
    return sizes[jax.random.permutation(jax.random.fold_in(rng, 2), amount)]


def normal_values(own_key, extent, deviation, limit, pieces=(), kind=jnp.bfloat16):
    gain = steps_of(own_key, extent, pieces, -0.22, 0.18) if pieces else 1.0
    drawn = jax.random.normal(own_key, extent, jnp.float32) * deviation * gain
    return jnp.minimum(jnp.maximum(drawn, -limit), limit).astype(kind)


def setup_inputs(seed: int = 0, part: int = 0) -> dict:
    arg_keys = jax.random.split(jax.random.key(seed), 18)
    part_keys = jax.random.split(jax.random.fold_in(arg_keys[17], part), 18)
    return {
        "piece_tokens": normal_values(part_keys[0], (PIECE, D), 1.0, 6.0, ((0, 4),)),
        "step_tokens": normal_values(part_keys[1], (DEC, D), 1.0, 6.0, ((0, 4),)),
        "norm_gain": jnp.clip(1.0 + 0.18 * jax.random.normal(arg_keys[2], (D,), jnp.float32), 0.1, 1.9),
        "query_weight": normal_values(arg_keys[3], (D, HEADS * HEAD), D ** -0.5, 0.125, ((1, 2),)),
        "key_weight": normal_values(arg_keys[4], (D, HEADS * HEAD), D ** -0.5, 0.125, ((1, 2),)),
        "value_weight": normal_values(arg_keys[5], (D, HEADS * HEAD), D ** -0.5, 0.125, ((1, 2),)),
        "gate_weight": normal_values(arg_keys[6], (D, HEADS), D ** -0.5, 0.125),
        "gate_bias": draw_gate_bias(jax.random.fold_in(arg_keys[17], 71), part),
        "out_weight": normal_values(arg_keys[8], (HEADS * HEAD, D), (HEADS * HEAD) ** -0.5, 0.1875, ((1, 2),)),
        "cache_keys": draw_cache_keys(jax.random.fold_in(jax.random.fold_in(arg_keys[17], part), 71), part),
        "cache_values": draw_cache_values(jax.random.fold_in(jax.random.fold_in(arg_keys[17], part), 71), part),
        "cache_decay": draw_cache_decay(jax.random.fold_in(jax.random.fold_in(arg_keys[17], part), 71), part),
        "decay_total": draw_decay_total(jax.random.fold_in(jax.random.fold_in(arg_keys[17], part), 71), part),
        "step_keys": normal_values(part_keys[13], (DEC, DEC_LEN, HEADS * HEAD), 1.0, 6.0, ((0, 4), (2, 2))),
        "step_values": normal_values(part_keys[14], (DEC, DEC_LEN, HEADS * HEAD), 1.0, 6.0, ((0, 4), (2, 2))),
        "step_gates": draw_step_gates(jax.random.fold_in(jax.random.fold_in(arg_keys[17], part), 71), part),
        "step_lengths": ragged(part_keys[16], DEC, DEC * DEC_LEN // 2, DEC_LEN, 2).astype(jnp.int32),
    }


norm_eps = 1e-06
negative = -1e+30

def normalize(token_rows, norm_gain):
    wide = token_rows.astype(jnp.float32)
    factor = lax.rsqrt(lax.optimization_barrier(jnp.mean(wide * wide, axis=-1, keepdims=True)) + norm_eps)
    return (wide * factor * norm_gain).astype(jnp.bfloat16)

def reference(piece_tokens, step_tokens, norm_gain, query_weight, key_weight, value_weight, gate_weight, gate_bias, out_weight, cache_keys, cache_values, cache_decay, decay_total, step_keys, step_values, step_gates, step_lengths):
    score_scale = HEAD ** (-0.5)
    token_rows = jnp.concatenate([piece_tokens, step_tokens], axis=0)
    normed = normalize(token_rows, norm_gain)
    queries = jnp.dot(normed, query_weight, preferred_element_type=jnp.float32).astype(jnp.bfloat16)
    new_keys = jnp.dot(normed, key_weight, preferred_element_type=jnp.float32).astype(jnp.bfloat16)
    new_values = jnp.dot(normed, value_weight, preferred_element_type=jnp.float32).astype(jnp.bfloat16)
    log_gates = jax.nn.log_sigmoid(jnp.dot(normed, gate_weight, preferred_element_type=jnp.float32) + gate_bias)
    piece_q = queries[:PIECE].reshape(PIECE, HEADS, HEAD).astype(jnp.float32)
    piece_k = new_keys[:PIECE].reshape(PIECE, HEADS, HEAD)
    piece_v = new_values[:PIECE].reshape(PIECE, HEADS, HEAD)
    piece_decay = decay_total[None, :] + jnp.cumsum(log_gates[:PIECE], axis=0)
    query_pos = jnp.arange(PIECE, dtype=jnp.int32)
    key_local = jnp.arange(PIECE_DEV, dtype=jnp.int32)

    def visit_block(carry_in, block_id):
        best_high, mass_sum, weighted = carry_in
        cache_start = (block_id * CACHE_DEV).astype(jnp.int32)
        piece_start = (block_id * PIECE_DEV).astype(jnp.int32)
        own_keys = lax.dynamic_slice_in_dim(cache_keys, cache_start, CACHE_DEV, 0).reshape(CACHE_DEV, HEADS, HEAD)
        own_values = lax.dynamic_slice_in_dim(cache_values, cache_start, CACHE_DEV, 0).reshape(CACHE_DEV, HEADS, HEAD)
        own_decay = lax.dynamic_slice_in_dim(cache_decay, cache_start, CACHE_DEV, 1)
        block_keys = lax.dynamic_slice_in_dim(piece_k, piece_start, PIECE_DEV, 0)
        block_values = lax.dynamic_slice_in_dim(piece_v, piece_start, PIECE_DEV, 0)
        block_decay = lax.dynamic_slice_in_dim(piece_decay, piece_start, PIECE_DEV, 0).T
        join_keys = jnp.concatenate([own_keys, block_keys], axis=0).astype(jnp.float32)
        join_values = jnp.concatenate([own_values, block_values], axis=0).astype(jnp.float32)
        join_decay = jnp.concatenate([own_decay, block_decay], axis=1)
        scores = jnp.einsum('qhd,khd->hqk', piece_q, join_keys) * score_scale
        scores = scores + piece_decay.T[:, :, None] - join_decay[:, None, :]
        visible = jnp.concatenate([jnp.ones((PIECE, CACHE_DEV), jnp.bool_), query_pos[:, None] >= (piece_start + key_local)[None, :]], axis=1)
        scores = jnp.where(visible[None], scores, negative)
        row_high = lax.optimization_barrier(jnp.max(scores, axis=-1))
        exp_scores = jnp.exp(scores - row_high[..., None])
        row_mass = lax.optimization_barrier(jnp.sum(exp_scores, axis=-1))
        block_weights = lax.optimization_barrier(exp_scores.astype(jnp.bfloat16)).astype(jnp.float32)
        block_means = (jnp.einsum('hqk,khd->hqd', block_weights, join_values) / row_mass[..., None]).astype(jnp.bfloat16)
        block_means = lax.optimization_barrier(block_means).astype(jnp.float32)
        new_best = jnp.maximum(best_high, row_high)
        keep_old = jnp.exp(best_high - new_best)
        add_new = row_mass * jnp.exp(row_high - new_best)
        mass_sum = mass_sum * keep_old + add_new
        weighted = weighted * keep_old[..., None] + add_new[..., None] * block_means
        return ((new_best, mass_sum, weighted), None)
    start_state = (jnp.full((HEADS, PIECE), negative, jnp.float32), jnp.zeros((HEADS, PIECE), jnp.float32), jnp.zeros((HEADS, PIECE, HEAD), jnp.float32))
    (best_high, mass_sum, weighted), unused = lax.scan(visit_block, start_state, jnp.arange(N_KV, dtype=jnp.int32))
    piece_att = (weighted / mass_sum[..., None]).astype(jnp.bfloat16).transpose(1, 0, 2).reshape(PIECE, HEADS * HEAD)
    step_q = queries[PIECE:].reshape(DEC, HEADS, HEAD).astype(jnp.float32)
    step_k = new_keys[PIECE:].reshape(DEC, HEADS, HEAD).astype(jnp.float32)
    step_v = new_values[PIECE:].reshape(DEC, HEADS, HEAD).astype(jnp.float32)
    step_lg = log_gates[PIECE:]
    in_cache = jnp.arange(DEC_LEN, dtype=jnp.int32)[None, :] < step_lengths[:, None]
    kept_gates = jnp.where(in_cache[:, None, :], step_gates, 0.0)
    after_sum = lax.cumsum(kept_gates, axis=2, reverse=True) - kept_gates
    cache_scores = jnp.einsum('bhd,blhd->bhl', step_q, step_keys.reshape(DEC, DEC_LEN, HEADS, HEAD).astype(jnp.float32)) * score_scale
    cache_scores = cache_scores + step_lg[:, :, None] + after_sum
    cache_scores = jnp.where(in_cache[:, None, :], cache_scores, negative)
    self_scores = lax.optimization_barrier(jnp.sum(step_q * step_k, axis=-1)) * score_scale
    step_high = jnp.maximum(lax.optimization_barrier(jnp.max(cache_scores, axis=-1)), self_scores)
    cache_exp = jnp.exp(cache_scores - step_high[..., None])
    self_exp = jnp.exp(self_scores - step_high)
    step_mass = lax.optimization_barrier(jnp.sum(cache_exp, axis=-1)) + self_exp
    cache_weights = lax.optimization_barrier(cache_exp.astype(jnp.bfloat16)).astype(jnp.float32)
    self_weights = lax.optimization_barrier(self_exp.astype(jnp.bfloat16)).astype(jnp.float32)
    step_mix = jnp.einsum('bhl,blhd->bhd', cache_weights, step_values.reshape(DEC, DEC_LEN, HEADS, HEAD).astype(jnp.float32))
    step_mix = step_mix + self_weights[..., None] * step_v
    step_att = (step_mix / step_mass[..., None]).astype(jnp.bfloat16).reshape(DEC, HEADS * HEAD)
    piece_out = jnp.dot(piece_att, out_weight, preferred_element_type=jnp.float32).astype(jnp.bfloat16)
    step_out = jnp.dot(step_att, out_weight, preferred_element_type=jnp.float32).astype(jnp.bfloat16)
    return (piece_out, step_out)
```

```python
import functools
import math

import jax
import jax.numpy as jnp
from jax import lax
from jax.experimental import pallas as pl
from jax.experimental.pallas import tpu as pltpu
from jax.sharding import PartitionSpec as P

norm_eps = 1e-06
negative = -1e30
log2e = math.log2(math.e)
MESH = pl.DeviceIdType.MESH
F32 = jnp.float32
BF16 = jnp.bfloat16
NT = (((1,), (1,)), ((), ()))
TN = (((0,), (0,)), ((), ()))


def iota(shape, dim):
    return lax.broadcasted_iota(jnp.int32, shape, dim)


def normalize(rows, gain):
    wide = rows.astype(F32)
    factor = lax.rsqrt(jnp.mean(wide * wide, axis=-1, keepdims=True) + norm_eps)
    return (wide * factor * gain).astype(BF16)


def to_column(row, count):
    eye = iota((count, count), 0) == iota((count, count), 1)
    return jnp.sum(jnp.where(eye, row, 0.0), axis=1, keepdims=True)


def kernel(
    n, heads, width,
    tok, stok, gain, gate_w, gate_b, total_decay, cache_decay, step_gates, step_len,
    wq, wk, wv, wo, cache_k, cache_v, step_k, step_v,
    out_piece, out_step,
    nrm, wq_v, wk_v, wv_v, wo_v, k_all, v_all, sk_v, sv_v,
    q_all, lg, gate_buf, key_bias, mean_buf, stat_buf, att, att_other,
    local_sem, q_send, q_recv, g_send, g_recv, m_send, m_recv, s_send, s_recv, x_send, x_recv,
):
    me = lax.axis_index("kv")
    tp = lax.axis_index("tp")
    rows = tok.shape[0]
    steps = stok.shape[0]
    cache_len = cache_k.shape[0]
    span = step_k.shape[0] // steps
    local = heads * width
    scale = width ** (-0.5) * log2e

    def fetch(index, src, dst):
        copy = pltpu.make_async_copy(src, dst, local_sem.at[index])
        copy.start()
        return copy

    c_wq = fetch(0, wq, wq_v)
    c_wk = fetch(1, wk, wk_v)
    c_wv = fetch(2, wv, wv_v)
    c_ck = fetch(3, cache_k, k_all.at[pl.ds(0, cache_len)])
    c_cv = fetch(4, cache_v, v_all.at[pl.ds(0, cache_len)])
    c_sk = fetch(5, step_k, sk_v)
    c_sv = fetch(6, step_v, sv_v)
    c_wo = fetch(7, wo, wo_v)

    barrier = pltpu.get_barrier_semaphore()

    def greet(d, carry):
        pl.semaphore_signal(
            barrier, inc=1, device_id={"kv": lax.rem(me + d, n)}, device_id_type=MESH
        )
        return carry

    lax.fori_loop(1, n, greet, 0)
    pl.semaphore_signal(barrier, inc=1, device_id={"tp": 1 - tp}, device_id_type=MESH)

    nrm[pl.ds(0, rows)] = normalize(tok[...], gain[...])
    pad = nrm.shape[0] - rows
    step_norm = normalize(stok[...], gain[...]).astype(F32)
    step_rows = jnp.zeros((pad, nrm.shape[1]), F32)
    for b in range(steps):
        step_rows = jnp.where(iota((pad, nrm.shape[1]), 0) == b, step_norm[b : b + 1], step_rows)
    nrm[pl.ds(rows, pad)] = step_rows.astype(BF16)

    c_wq.wait()
    q_new = jnp.dot(nrm[...], wq_v[...], preferred_element_type=F32).astype(BF16)
    q_all[0] = q_new[:rows]
    step_q = q_new[rows:].astype(F32)

    pl.semaphore_wait(barrier, n)

    def q_copy(d):
        return pltpu.make_async_remote_copy(
            src_ref=q_all.at[0], dst_ref=q_all.at[d],
            send_sem=q_send.at[d], recv_sem=q_recv.at[d],
            device_id={"kv": lax.rem(me + d, n)}, device_id_type=MESH,
        )

    def g_copy(d):
        return pltpu.make_async_remote_copy(
            src_ref=gate_buf.at[0], dst_ref=gate_buf.at[d],
            send_sem=g_send.at[d], recv_sem=g_recv.at[d],
            device_id={"kv": lax.rem(me + d, n)}, device_id_type=MESH,
        )

    def m_copy(d):
        return pltpu.make_async_remote_copy(
            src_ref=mean_buf.at[n + d], dst_ref=mean_buf.at[d],
            send_sem=m_send.at[d], recv_sem=m_recv.at[d],
            device_id={"kv": lax.rem(me + n - d, n)}, device_id_type=MESH,
        )

    def s_copy(d):
        return pltpu.make_async_remote_copy(
            src_ref=stat_buf.at[n + d], dst_ref=stat_buf.at[d],
            send_sem=s_send.at[d], recv_sem=s_recv.at[d],
            device_id={"kv": lax.rem(me + n - d, n)}, device_id_type=MESH,
        )

    def each(make):
        def body(d, carry):
            make(d)
            return carry

        lax.fori_loop(1, n, body, 0)

    each(lambda d: q_copy(d).start())

    logits = lax.dot_general(gate_w[...], nrm[...], NT, preferred_element_type=F32)
    logits = logits + to_column(gate_b[...], gate_w.shape[0])
    lg[...] = jnp.minimum(logits, 0.0) - jnp.log1p(jnp.exp(-jnp.abs(logits)))
    own_lg = lg[pl.ds(pl.multiple_of(tp * heads, heads), heads), :]
    piece_lg = own_lg[:, :rows]
    gate_buf[0] = jnp.broadcast_to(jnp.sum(piece_lg, axis=1, keepdims=True), gate_buf.shape[1:])
    each(lambda d: g_copy(d).start())

    c_wk.wait()
    k_new = jnp.dot(nrm[...], wk_v[...], preferred_element_type=F32).astype(BF16)
    k_all[pl.ds(cache_len, rows)] = k_new[:rows]
    step_nk = k_new[rows:].astype(F32)
    c_wv.wait()
    v_new = jnp.dot(nrm[...], wv_v[...], preferred_element_type=F32).astype(BF16)
    v_all[pl.ds(cache_len, rows)] = v_new[:rows]
    step_nv = v_new[rows:].astype(F32)

    upto = (iota((rows, rows), 0) <= iota((rows, rows), 1)).astype(F32)
    running = jnp.dot(
        piece_lg, upto, preferred_element_type=F32, precision=lax.Precision.HIGHEST
    )
    lg_start = to_column(total_decay[...], gate_w.shape[0])
    tp_pick = iota(lg_start.shape, 0)
    start_rows = jnp.where(tp == 0, lg_start[:heads], lg_start[heads : 2 * heads])
    key_bias[:, pl.ds(0, cache_len)] = (start_rows - cache_decay[...]) * log2e

    def add_before(d, total):
        g_copy(d).wait()
        return total + jnp.where(d <= me, gate_buf[d], 0.0)

    before = lax.fori_loop(1, n, add_before, jnp.zeros(gate_buf.shape[1:], F32))
    key_bias[:, pl.ds(cache_len, rows)] = -(before[:, :1] + running) * log2e
    c_ck.wait()
    c_cv.wait()

    pair_lanes = 2 * width
    low_lane = iota((rows, pair_lanes), 1) < width
    stat_lane = iota((rows, 128), 1)
    row_minus_col = iota((rows, rows), 0) - iota((rows, rows), 1)

    def attend(i, carry):
        odd = lax.rem(i, 2)
        d = odd * lax.div(i + 1, 2) + (1 - odd) * lax.rem(n - lax.div(i, 2), n)

        @pl.when(i > 0)
        def _():
            q_copy(d).wait_recv()

        source = lax.rem(me - d + n, n)
        slot = d + n * jnp.minimum(i, 1)
        visible = row_minus_col >= (me - source) * rows
        stats = jnp.zeros((rows, 128), F32)
        for pair in range(heads // 2):
            lanes = pl.ds(pair * pair_lanes, pair_lanes)
            q_pair = q_all[d, :, lanes]
            keys = k_all[:, lanes]
            values = v_all[:, lanes]
            outs = []
            for side in range(2):
                head = 2 * pair + side
                keep = low_lane if side == 0 else jnp.logical_not(low_lane)
                q_one = jnp.where(keep, q_pair, jnp.zeros_like(q_pair))
                scores = lax.dot_general(q_one, keys, NT, preferred_element_type=F32)
                scores = scores * scale + key_bias[head : head + 1, :]
                fresh = jnp.where(visible, scores[:, cache_len:], negative)
                scores = jnp.concatenate([scores[:, :cache_len], fresh], axis=1)
                high = jnp.max(scores, axis=1, keepdims=True)
                weight = jnp.exp2(scores - high)
                mass = jnp.sum(weight, axis=1, keepdims=True)
                mix = jnp.dot(weight.astype(BF16), values, preferred_element_type=F32)
                outs.append(mix / mass)
                stats = jnp.where(stat_lane == head, high, stats)
                stats = jnp.where(stat_lane == heads + head, mass, stats)
            mean_buf[slot, :, lanes] = jnp.where(low_lane, outs[0], outs[1]).astype(BF16)
        stat_buf[slot] = stats.T[: 2 * heads]

        @pl.when(i > 0)
        def _():
            m_copy(d).start()
            s_copy(d).start()

        return carry

    lax.fori_loop(0, n, attend, 0)

    head_mask = lax.div(iota((heads, local), 1), width) == iota((heads, local), 0)
    chunk = 128
    chunks = span // chunk
    later = (iota((chunk, chunk), 0) > iota((chunk, chunk), 1)).astype(F32)
    c_sk.wait()
    c_sv.wait()
    step_att = jnp.zeros((pad, local), F32)
    for b in range(steps):
        length = step_len[b]
        in_cache = iota((heads, span), 1) < length
        kept = jnp.where(in_cache, step_gates[b], 0.0)
        tail = jnp.zeros((heads, 1), F32)
        parts = [None] * chunks
        for c in reversed(range(chunks)):
            piece = kept[:, c * chunk : (c + 1) * chunk]
            inner = jnp.dot(
                piece, later, preferred_element_type=F32, precision=lax.Precision.HIGHEST
            )
            parts[c] = inner + tail
            tail = tail + jnp.sum(piece, axis=1, keepdims=True)
        after = jnp.concatenate(parts, axis=1)
        q_row = jnp.where(head_mask, step_q[b : b + 1], 0.0)
        scores = lax.dot_general(
            q_row.astype(BF16), sk_v[pl.ds(b * span, span)], NT, preferred_element_type=F32
        )
        new_lg = own_lg[:, rows + b : rows + b + 1]
        scores = scores * scale + (new_lg + after) * log2e
        scores = jnp.where(in_cache, scores, negative)
        self_score = jnp.sum(q_row * step_nk[b : b + 1], axis=1, keepdims=True) * scale
        high = jnp.maximum(jnp.max(scores, axis=1, keepdims=True), self_score)
        weight = jnp.exp2(scores - high)
        self_weight = jnp.exp2(self_score - high)
        mass = jnp.sum(weight, axis=1, keepdims=True) + self_weight
        mix = jnp.dot(
            weight.astype(BF16), sv_v[pl.ds(b * span, span)], preferred_element_type=F32
        )
        mix = mix + self_weight.astype(BF16).astype(F32) * step_nv[b : b + 1]
        one = jnp.sum(jnp.where(head_mask, mix / mass, 0.0), axis=0, keepdims=True)
        step_att = jnp.where(iota((pad, local), 0) == b, one, step_att)
    att[pl.ds(rows, pad)] = step_att.astype(BF16)

    def top(d, best):
        s_copy(d).wait()
        return jnp.maximum(best, stat_buf[d, :heads])

    best = lax.fori_loop(1, n, top, stat_buf[0, :heads])

    def share_of(d):
        return stat_buf[d, pl.ds(heads, heads)] * jnp.exp2(stat_buf[d, :heads] - best)

    total = lax.fori_loop(1, n, lambda d, t: t + share_of(d), share_of(0))
    spread = head_mask.astype(F32)

    def weighted(d):
        wide = lax.dot_general(
            share_of(d) / total, spread, TN,
            preferred_element_type=F32, precision=lax.Precision.HIGHEST,
        )
        return wide * mean_buf[d].astype(F32)

    def add_block(d, acc):
        m_copy(d).wait()
        return acc + weighted(d)

    att[pl.ds(0, rows)] = lax.fori_loop(1, n, add_block, weighted(0)).astype(BF16)

    swap = pltpu.make_async_remote_copy(
        src_ref=att, dst_ref=att_other, send_sem=x_send, recv_sem=x_recv,
        device_id={"tp": 1 - tp}, device_id_type=MESH,
    )
    swap.start()
    c_wo.wait()
    mine = pl.ds(pl.multiple_of(tp * local, local), local)
    other = pl.ds(pl.multiple_of((1 - tp) * local, local), local)
    projected = jnp.dot(att[...], wo_v[mine, :], preferred_element_type=F32)
    swap.wait()
    projected = projected + jnp.dot(att_other[...], wo_v[other, :], preferred_element_type=F32)
    out_piece[...] = projected[:rows].astype(BF16)
    out_step[...] = projected[rows : rows + steps].astype(BF16)
    each(lambda d: q_copy(d).wait_send())


def per_device(
    piece_tokens, step_tokens, norm_gain, query_weight, key_weight, value_weight,
    gate_weight, gate_bias, out_weight, cache_keys, cache_values, cache_decay,
    decay_total, step_keys, step_values, step_gates, step_lengths,
):
    n = lax.axis_size("kv")
    rows, model = piece_tokens.shape
    steps = step_tokens.shape[0]
    heads = cache_decay.shape[0]
    local = query_weight.shape[1]
    width = local // heads
    cache_len = cache_keys.shape[0]
    span = step_keys.shape[1]
    columns = out_weight.shape[1]
    padded = rows + 16 * (-(-steps // 16))
    vmem = pl.BlockSpec(memory_space=pltpu.VMEM)
    smem = pl.BlockSpec(memory_space=pltpu.SMEM)
    hbm = pl.BlockSpec(memory_space=pl.ANY)
    dma = pltpu.SemaphoreType.DMA
    piece_out, step_out = pl.pallas_call(
        functools.partial(kernel, n, heads, width),
        out_shape=(
            jax.ShapeDtypeStruct((rows, columns), BF16),
            jax.ShapeDtypeStruct((steps, columns), BF16),
        ),
        in_specs=[vmem] * 8 + [smem] + [hbm] * 8,
        out_specs=(vmem, vmem),
        scratch_shapes=[
            pltpu.VMEM((padded, model), BF16),
            pltpu.VMEM(query_weight.shape, BF16),
            pltpu.VMEM(key_weight.shape, BF16),
            pltpu.VMEM(value_weight.shape, BF16),
            pltpu.VMEM(out_weight.shape, BF16),
            pltpu.VMEM((cache_len + rows, local), BF16),
            pltpu.VMEM((cache_len + rows, local), BF16),
            pltpu.VMEM((steps * span, local), BF16),
            pltpu.VMEM((steps * span, local), BF16),
            pltpu.VMEM((n, rows, local), BF16),
            pltpu.VMEM((gate_weight.shape[1], padded), F32),
            pltpu.VMEM((n, heads, 128), F32),
            pltpu.VMEM((heads, cache_len + rows), F32),
            pltpu.VMEM((2 * n, rows, local), BF16),
            pltpu.VMEM((2 * n, 2 * heads, rows), F32),
            pltpu.VMEM((padded, local), BF16),
            pltpu.VMEM((padded, local), BF16),
            dma((8,)),
            dma((n,)), dma((n,)), dma((n,)), dma((n,)),
            dma((n,)), dma((n,)), dma((n,)), dma((n,)),
            dma(()), dma(()),
        ],
        compiler_params=pltpu.CompilerParams(
            collective_id=0, has_side_effects=True, vmem_limit_bytes=60 * 1024 * 1024
        ),
    )(
        piece_tokens, step_tokens, norm_gain.reshape(1, -1), gate_weight.T,
        gate_bias.reshape(1, -1), decay_total.reshape(1, -1), cache_decay, step_gates,
        step_lengths, query_weight, key_weight, value_weight, out_weight,
        cache_keys, cache_values,
        step_keys.reshape(steps * span, local), step_values.reshape(steps * span, local),
    )
    return piece_out, step_out


def solution(mesh):
    rows = P(("dp", "kv"), None)
    both = P(("dp", "kv"), "tp")
    cols = P(None, "tp")
    in_specs = (
        rows, rows, P(), cols, cols, cols, P(), P(), cols, both, both,
        P("tp", ("dp", "kv")), P("dp"),
        P(("dp", "kv"), None, "tp"), P(("dp", "kv"), None, "tp"),
        P(("dp", "kv"), "tp", None), P(("dp", "kv")),
    )
    return jax.shard_map(
        per_device, mesh=mesh, in_specs=in_specs, out_specs=(both, both), check_vma=False
    )
```

```python
import functools
import math

import jax
import jax.numpy as jnp
from jax import lax
from jax.experimental import pallas as pl
from jax.experimental.pallas import tpu as pltpu
from jax.sharding import PartitionSpec as P

norm_eps = 1e-06
negative = -1e30
log2e = math.log2(math.e)
MESH = pl.DeviceIdType.MESH
F32 = jnp.float32
BF16 = jnp.bfloat16
NT = (((1,), (1,)), ((), ()))
TN = (((0,), (0,)), ((), ()))


chunk_count = 2


def iota(shape, dim):
    return lax.broadcasted_iota(jnp.int32, shape, dim)


def normalize(rows, gain):
    wide = rows.astype(F32)
    factor = lax.rsqrt(jnp.mean(wide * wide, axis=-1, keepdims=True) + norm_eps)
    return (wide * factor * gain).astype(BF16)


def to_column(row, count):
    eye = iota((count, count), 0) == iota((count, count), 1)
    return jnp.sum(jnp.where(eye, row, 0.0), axis=1, keepdims=True)


def kernel(
    n, heads, width,
    tok, stok, gain, gate_w, gate_b, total_decay, cache_decay, step_gates, step_len,
    wq, wk, wv, cache_k, cache_v, step_k, step_v,
    out_att,
    nrm, wq_v, wk_v, wv_v, k_all, k_turned, v_all, sk_v, sv_v,
    q_all, lg, gate_buf, key_bias, mean_buf, stat_buf, att, att_other,
    local_sem, q_right, q_left, q_recv, g_send, g_recv, m_send, m_recv, s_send, s_recv, x_send, x_recv,
):
    me = lax.axis_index("kv")
    tp = lax.axis_index("tp")
    rows = tok.shape[0]
    steps = stok.shape[0]
    cache_len = cache_k.shape[0]
    span = step_k.shape[0] // steps
    local = heads * width
    scale = width ** (-0.5) * log2e

    def fetch(index, src, dst):
        copy = pltpu.make_async_copy(src, dst, local_sem.at[index])
        copy.start()
        return copy

    c_wq = fetch(0, wq, wq_v)
    c_wk = fetch(1, wk, wk_v)
    c_wv = fetch(2, wv, wv_v)
    c_ck = fetch(3, cache_k, k_all)
    c_cv = fetch(4, cache_v, v_all.at[pl.ds(0, cache_len)])
    c_sk = fetch(5, step_k, sk_v)
    c_sv = fetch(6, step_v, sv_v)

    barrier = pltpu.get_barrier_semaphore()

    def greet(d, carry):
        pl.semaphore_signal(
            barrier, inc=1, device_id={"kv": lax.rem(me + d, n)}, device_id_type=MESH
        )
        return carry

    lax.fori_loop(1, n, greet, 0)
    pl.semaphore_signal(barrier, inc=1, device_id={"tp": 1 - tp}, device_id_type=MESH)

    nrm[pl.ds(0, rows)] = normalize(tok[...], gain[...])
    pad = nrm.shape[0] - rows
    step_norm = normalize(stok[...], gain[...]).astype(F32)
    step_rows = jnp.zeros((pad, nrm.shape[1]), F32)
    for b in range(steps):
        step_rows = jnp.where(iota((pad, nrm.shape[1]), 0) == b, step_norm[b : b + 1], step_rows)
    nrm[pl.ds(rows, pad)] = step_rows.astype(BF16)

    c_wq.wait()
    q_new = jnp.dot(nrm[...], wq_v[...], preferred_element_type=F32).astype(BF16)
    part = local // chunk_count
    for c in range(chunk_count):
        q_all[me, c] = q_new[:rows, c * part : (c + 1) * part]
    step_q = q_new[rows:].astype(F32)

    pl.semaphore_wait(barrier, n)

    def q_copy(source, c, step, sems):
        return pltpu.make_async_remote_copy(
            src_ref=q_all.at[source, c], dst_ref=q_all.at[source, c],
            send_sem=sems.at[source, c], recv_sem=q_recv.at[source, c],
            device_id={"kv": lax.rem(me + step + n, n)}, device_id_type=MESH,
        )

    def to_right(source, c):
        return q_copy(source, c, 1, q_right)

    def to_left(source, c):
        return q_copy(source, c, -1, q_left)

    has_right = me < n - 1
    has_left = me > 0

    def g_copy(d):
        return pltpu.make_async_remote_copy(
            src_ref=gate_buf.at[0], dst_ref=gate_buf.at[d],
            send_sem=g_send.at[d], recv_sem=g_recv.at[d],
            device_id={"kv": lax.rem(me + d, n)}, device_id_type=MESH,
        )

    def m_copy(d):
        return pltpu.make_async_remote_copy(
            src_ref=mean_buf.at[n + d], dst_ref=mean_buf.at[d],
            send_sem=m_send.at[d], recv_sem=m_recv.at[d],
            device_id={"kv": lax.rem(me + n - d, n)}, device_id_type=MESH,
        )

    def s_copy(d):
        return pltpu.make_async_remote_copy(
            src_ref=stat_buf.at[n + d], dst_ref=stat_buf.at[d],
            send_sem=s_send.at[d], recv_sem=s_recv.at[d],
            device_id={"kv": lax.rem(me + n - d, n)}, device_id_type=MESH,
        )

    def each(make):
        def body(d, carry):
            make(d)
            return carry

        lax.fori_loop(1, n, body, 0)

    for c in range(chunk_count):
        @pl.when(has_right)
        def _():
            to_right(me, c).start()

        @pl.when(has_left)
        def _():
            to_left(me, c).start()

    logits = lax.dot_general(gate_w[...], nrm[...], NT, preferred_element_type=F32)
    logits = logits + to_column(gate_b[...], gate_w.shape[0])
    lg[...] = jnp.minimum(logits, 0.0) - jnp.log1p(jnp.exp(-jnp.abs(logits)))
    own_lg = lg[pl.ds(pl.multiple_of(tp * heads, heads), heads), :]
    piece_lg = own_lg[:, :rows]
    gate_buf[0] = jnp.broadcast_to(jnp.sum(piece_lg, axis=1, keepdims=True), gate_buf.shape[1:])
    each(lambda d: g_copy(d).start())

    c_ck.wait()
    k_turned[:, pl.ds(0, cache_len)] = k_all[...].T
    c_wk.wait()
    k_new = jnp.dot(nrm[...], wk_v[...], preferred_element_type=F32).astype(BF16)
    k_turned[:, pl.ds(cache_len, rows)] = k_new[:rows].T
    step_nk = k_new[rows:].astype(F32)
    c_wv.wait()
    v_new = jnp.dot(nrm[...], wv_v[...], preferred_element_type=F32).astype(BF16)
    v_all[pl.ds(cache_len, rows)] = v_new[:rows]
    step_nv = v_new[rows:].astype(F32)

    upto = (iota((rows, rows), 0) <= iota((rows, rows), 1)).astype(F32)
    running = jnp.dot(
        piece_lg, upto, preferred_element_type=F32, precision=lax.Precision.HIGHEST
    )
    lg_start = to_column(total_decay[...], gate_w.shape[0])
    start_rows = jnp.where(tp == 0, lg_start[:heads], lg_start[heads : 2 * heads])
    key_bias[:, pl.ds(0, cache_len)] = (start_rows - cache_decay[...]) * log2e

    def add_before(d, total):
        g_copy(d).wait()
        return total + jnp.where(d <= me, gate_buf[d], 0.0)

    before = lax.fori_loop(1, n, add_before, jnp.zeros(gate_buf.shape[1:], F32))
    key_bias[:, pl.ds(cache_len, rows)] = -(before[:, :1] + running) * log2e

    pair_lanes = 2 * width
    low_lane = iota((rows, pair_lanes), 1) < width
    stat_lane = iota((rows, 128), 1)
    row_minus_col = iota((rows, rows), 0) - iota((rows, rows), 1)

    c_cv.wait()

    def attend(d, source, remote):
        slot = d + n if remote else d
        visible = row_minus_col >= (me - source) * rows
        stats = jnp.zeros((rows, 128), F32)
        pairs_in_part = heads // 2 // chunk_count
        for pair in range(heads // 2):
            lanes = pl.ds(pair * pair_lanes, pair_lanes)
            inner = pl.ds(pair % pairs_in_part * pair_lanes, pair_lanes)
            q_pair = q_all[source, pair // pairs_in_part, :, inner]
            keys = k_turned[lanes, :]
            values = v_all[:, lanes]
            outs = []
            for side in range(2):
                head = 2 * pair + side
                keep = low_lane if side == 0 else jnp.logical_not(low_lane)
                q_one = jnp.where(keep, q_pair, jnp.zeros_like(q_pair))
                scores = jnp.dot(q_one, keys, preferred_element_type=F32)
                scores = scores * scale + key_bias[head : head + 1, :]
                fresh = jnp.where(visible, scores[:, cache_len:], negative)
                scores = jnp.concatenate([scores[:, :cache_len], fresh], axis=1)
                high = jnp.max(scores, axis=1, keepdims=True)
                weight = jnp.exp2(scores - high)
                mass = jnp.sum(weight, axis=1, keepdims=True)
                mix = jnp.dot(weight.astype(BF16), values, preferred_element_type=F32)
                outs.append(mix / mass)
                stats = jnp.where(stat_lane == head, high, stats)
                stats = jnp.where(stat_lane == heads + head, mass, stats)
            mean_buf[slot, :, lanes] = jnp.where(low_lane, outs[0], outs[1]).astype(BF16)
        stat_buf[slot] = stats.T[: 2 * heads]
        if remote:
            m_copy(d).start()
            s_copy(d).start()

    def step(k, carry):
        for c in range(chunk_count):
            @pl.when(me >= k)
            def _():
                to_right(me - k, c).wait_recv()

                @pl.when(has_right)
                def _():
                    to_right(me - k, c).start()

            @pl.when(me + k < n)
            def _():
                to_left(me + k, c).wait_recv()

                @pl.when(has_left)
                def _():
                    to_left(me + k, c).start()

        @pl.when(me >= k)
        def _():
            attend(k, me - k, True)

        @pl.when(me + k < n)
        def _():
            attend(n - k, me + k, True)

        @pl.when(k == 1)
        def _():
            attend(0, me, False)

        return carry

    lax.fori_loop(1, n, step, 0)

    head_mask = lax.div(iota((heads, local), 1), width) == iota((heads, local), 0)
    chunk = 128
    chunks = span // chunk
    later = (iota((chunk, chunk), 0) > iota((chunk, chunk), 1)).astype(F32)
    c_sk.wait()
    c_sv.wait()
    step_att = jnp.zeros((pad, local), F32)
    for b in range(steps):
        length = step_len[b]
        in_cache = iota((heads, span), 1) < length
        kept = jnp.where(in_cache, step_gates[b], 0.0)
        tail = jnp.zeros((heads, 1), F32)
        parts = [None] * chunks
        for c in reversed(range(chunks)):
            piece = kept[:, c * chunk : (c + 1) * chunk]
            inner = jnp.dot(
                piece, later, preferred_element_type=F32, precision=lax.Precision.HIGHEST
            )
            parts[c] = inner + tail
            tail = tail + jnp.sum(piece, axis=1, keepdims=True)
        after = jnp.concatenate(parts, axis=1)
        q_row = jnp.where(head_mask, step_q[b : b + 1], 0.0)
        scores = lax.dot_general(
            q_row.astype(BF16), sk_v[pl.ds(b * span, span)], NT, preferred_element_type=F32
        )
        new_lg = own_lg[:, rows + b : rows + b + 1]
        scores = scores * scale + (new_lg + after) * log2e
        scores = jnp.where(in_cache, scores, negative)
        self_score = jnp.sum(q_row * step_nk[b : b + 1], axis=1, keepdims=True) * scale
        high = jnp.maximum(jnp.max(scores, axis=1, keepdims=True), self_score)
        weight = jnp.exp2(scores - high)
        self_weight = jnp.exp2(self_score - high)
        mass = jnp.sum(weight, axis=1, keepdims=True) + self_weight
        mix = jnp.dot(
            weight.astype(BF16), sv_v[pl.ds(b * span, span)], preferred_element_type=F32
        )
        mix = mix + self_weight.astype(BF16).astype(F32) * step_nv[b : b + 1]
        one = jnp.sum(jnp.where(head_mask, mix / mass, 0.0), axis=0, keepdims=True)
        step_att = jnp.where(iota((pad, local), 0) == b, one, step_att)
    att[pl.ds(rows, pad)] = step_att.astype(BF16)

    def top(d, best):
        s_copy(d).wait()
        return jnp.maximum(best, stat_buf[d, :heads])

    best = lax.fori_loop(1, n, top, stat_buf[0, :heads])

    def share_of(d):
        return stat_buf[d, pl.ds(heads, heads)] * jnp.exp2(stat_buf[d, :heads] - best)

    total = lax.fori_loop(1, n, lambda d, t: t + share_of(d), share_of(0))
    spread = head_mask.astype(F32)

    def weighted(d):
        wide = lax.dot_general(
            share_of(d) / total, spread, TN,
            preferred_element_type=F32, precision=lax.Precision.HIGHEST,
        )
        return wide * mean_buf[d].astype(F32)

    def add_block(d, acc):
        m_copy(d).wait()
        return acc + weighted(d)

    att[pl.ds(0, rows)] = lax.fori_loop(1, n, add_block, weighted(0)).astype(BF16)

    swap = pltpu.make_async_remote_copy(
        src_ref=att, dst_ref=att_other, send_sem=x_send, recv_sem=x_recv,
        device_id={"tp": 1 - tp}, device_id_type=MESH,
    )
    swap.start()
    mine = pl.ds(pl.multiple_of(tp * local, local), local)
    other = pl.ds(pl.multiple_of((1 - tp) * local, local), local)
    out_att[:, mine] = att[...]
    swap.wait()
    out_att[:, other] = att_other[...]

    def sent(source, carry):
        for c in range(chunk_count):
            @pl.when(jnp.logical_and(has_right, source <= me))
            def _():
                to_right(source, c).wait_send()

            @pl.when(jnp.logical_and(has_left, source >= me))
            def _():
                to_left(source, c).wait_send()

        return carry

    lax.fori_loop(0, n, sent, 0)


def project(rows, att, weight, out_piece, out_step):
    projected = jnp.dot(att[...], weight[...], preferred_element_type=F32)
    out_piece[...] = projected[:rows].astype(BF16)
    out_step[...] = projected[rows : rows + out_step.shape[0]].astype(BF16)


def per_device(
    piece_tokens, step_tokens, norm_gain, query_weight, key_weight, value_weight,
    gate_weight, gate_bias, out_weight, cache_keys, cache_values, cache_decay,
    decay_total, step_keys, step_values, step_gates, step_lengths,
):
    n = lax.axis_size("kv")
    rows, model = piece_tokens.shape
    steps = step_tokens.shape[0]
    heads = cache_decay.shape[0]
    local = query_weight.shape[1]
    width = local // heads
    cache_len = cache_keys.shape[0]
    span = step_keys.shape[1]
    columns = out_weight.shape[1]
    padded = rows + 16 * (-(-steps // 16))
    vmem = pl.BlockSpec(memory_space=pltpu.VMEM)
    smem = pl.BlockSpec(memory_space=pltpu.SMEM)
    hbm = pl.BlockSpec(memory_space=pltpu.HBM)
    dma = pltpu.SemaphoreType.DMA
    att = pl.pallas_call(
        functools.partial(kernel, n, heads, width),
        out_shape=jax.ShapeDtypeStruct((padded, out_weight.shape[0]), BF16),
        in_specs=[vmem] * 8 + [smem] + [hbm] * 7,
        out_specs=vmem,
        scratch_shapes=[
            pltpu.VMEM((padded, model), BF16),
            pltpu.VMEM(query_weight.shape, BF16),
            pltpu.VMEM(key_weight.shape, BF16),
            pltpu.VMEM(value_weight.shape, BF16),
            pltpu.VMEM((cache_len, local), BF16),
            pltpu.VMEM((local, cache_len + rows), BF16),
            pltpu.VMEM((cache_len + rows, local), BF16),
            pltpu.VMEM((steps * span, local), BF16),
            pltpu.VMEM((steps * span, local), BF16),
            pltpu.VMEM((n, chunk_count, rows, local // chunk_count), BF16),
            pltpu.VMEM((gate_weight.shape[1], padded), F32),
            pltpu.VMEM((n, heads, 128), F32),
            pltpu.VMEM((heads, cache_len + rows), F32),
            pltpu.VMEM((2 * n, rows, local), BF16),
            pltpu.VMEM((2 * n, 2 * heads, rows), F32),
            pltpu.VMEM((padded, local), BF16),
            pltpu.VMEM((padded, local), BF16),
            dma((7,)),
            dma((n, chunk_count)), dma((n, chunk_count)), dma((n, chunk_count)),
            dma((n,)), dma((n,)),
            dma((n,)), dma((n,)), dma((n,)), dma((n,)),
            dma(()), dma(()),
        ],
        compiler_params=pltpu.CompilerParams(
            collective_id=0, has_side_effects=True, vmem_limit_bytes=60 * 1024 * 1024
        ),
    )(
        piece_tokens, step_tokens, norm_gain.reshape(1, -1), gate_weight.T,
        gate_bias.reshape(1, -1), decay_total.reshape(1, -1), cache_decay, step_gates,
        step_lengths, query_weight, key_weight, value_weight,
        cache_keys, cache_values,
        step_keys.reshape(steps * span, local), step_values.reshape(steps * span, local),
    )
    return pl.pallas_call(
        functools.partial(project, rows),
        out_shape=(
            jax.ShapeDtypeStruct((rows, columns), BF16),
            jax.ShapeDtypeStruct((steps, columns), BF16),
        ),
        in_specs=[vmem, vmem],
        out_specs=(vmem, vmem),
        compiler_params=pltpu.CompilerParams(vmem_limit_bytes=16 * 1024 * 1024),
    )(att, out_weight)


def solution(mesh):
    rows = P(("dp", "kv"), None)
    both = P(("dp", "kv"), "tp")
    cols = P(None, "tp")
    in_specs = (
        rows, rows, P(), cols, cols, cols, P(), P(), cols, both, both,
        P("tp", ("dp", "kv")), P("dp"),
        P(("dp", "kv"), None, "tp"), P(("dp", "kv"), None, "tp"),
        P(("dp", "kv"), "tp", None), P(("dp", "kv")),
    )
    return jax.shard_map(
        per_device, mesh=mesh, in_specs=in_specs, out_specs=(both, both), check_vma=False
    )
```
